32 devices in a mesh: ep: 8 (over z, core), tp: 4 (over y, x).
Axes of the slice: x: 2, y: 2, z: 4, core: 2. Of those that a mesh axis runs over, the one named last changes fastest.
Arguments:
- tokens: bfloat16 [2048, 2048], P('ep'), may hold values from -6 to 6
- gate_proj: bfloat16 [8, 2048, 4096], P('ep', None, 'tp'), may hold values from -0.125 to 0.125
- up_proj: bfloat16 [8, 2048, 4096], P('ep', None, 'tp'), may hold values from -0.125 to 0.125
- down_proj: bfloat16 [8, 4096, 2048], P('ep', 'tp'), may hold values from -0.09375 to 0.09375
- side_input_weight: bfloat16 [2048, 1024], P(None, 'tp'), may hold values from -0.125 to 0.125
- dense_out: bfloat16 [1024, 2048], P(None, 'tp'), may hold values from -0.1875 to 0.1875
- dense_gate: bfloat16 [2048], replicated, may hold values from -0.125 to 0.125
- chosen_rows: int32 [8, 256], P(None, 'ep'), may hold values from 0 to 255, as said below
- choice_weights: float32 [8, 256], P(None, 'ep'), may hold values from 0.25 to 1
Outputs:
- mixed: bfloat16 [2048, 2048], P('ep', 'tp')
The draws below stay inside these ranges and needn't reach their ends.
Inputs may be any that keep to these rules, and one draw needn't show every extreme that they name: `chosen_rows`: for each expert and each block of 32 columns (one index of ep), the 32 rows are distinct rows of that index's 256 tokens; every expert reads exactly 32 tokens of every index.
All inputs are finite; a program needn't handle non-finite values.
Results may differ from the reference program's by a relative error of at most 0.015.
Values may be sent and summed in bfloat16 or wider, within the bound.
A program may use at most 64 MiB of HBM per device.

```python
import jax
import jax.numpy as jnp
from jax import lax

D = 2048
FF = 4096
DENSE_FF = 1024
TOK_DEV = 256
SLOT = 32
EXPERTS = 8
CAP = 256
TOKENS = 2048
N_TP = 4


def draw_chosen_rows(key, part):
    block_list = TOKENS // TOK_DEV
    keys = jax.random.split(jax.random.fold_in(key, 17), EXPERTS * block_list)
    orders = jax.vmap(lambda k: jax.random.permutation(k, TOK_DEV))(keys)
    picked = orders[:, :SLOT].astype(jnp.int32)
    return picked.reshape(EXPERTS, block_list * SLOT)


def level_of(stream_key, extent, shards, least, largest):
    def one(axis_at, parts):
        draws = jax.random.uniform(jax.random.fold_in(jax.random.fold_in(stream_key, 6), axis_at), (parts,), jnp.float32, least / len(shards), largest / len(shards))
        return jnp.repeat(jnp.exp(draws), extent[axis_at] // parts).reshape((-1,) + (1,) * (len(extent) - axis_at - 1))

    level = one(*shards[0])
    for cut in shards[1:]:
        level = level * one(*cut)
    return level


def gaussian(rng, dims, width, bound, cuts=(), dtype=jnp.bfloat16):
    factor_of = level_of(rng, dims, cuts, -0.22, 0.18) if cuts else 1.0
    values = jax.random.normal(rng, dims, jnp.float32) * width * factor_of
    return jnp.minimum(jnp.maximum(values, -bound), bound).astype(dtype)


def setup_inputs(seed: int = 0) -> dict:
    splits = jax.random.split(jax.random.key(seed), 10)
    return {
        "tokens": gaussian(splits[0], (TOKENS, D), 1.0, 6.0, ((0, 8),)),
        "gate_proj": gaussian(splits[1], (EXPERTS, D, FF), D ** -0.5, 0.125, ((0, 8), (2, 4))),
        "up_proj": gaussian(splits[2], (EXPERTS, D, FF), D ** -0.5, 0.125, ((0, 8), (2, 4))),
        "down_proj": gaussian(splits[3], (EXPERTS, FF, D), FF ** -0.5, 0.09375, ((0, 8), (1, 4))),
        "side_input_weight": gaussian(splits[4], (D, DENSE_FF), D ** -0.5, 0.125, ((1, 4),)),
        "dense_out": gaussian(splits[5], (DENSE_FF, D), DENSE_FF ** -0.5, 0.1875, ((1, 4),)),
        "dense_gate": gaussian(splits[6], (D,), D ** -0.5, 0.125),
        "chosen_rows": draw_chosen_rows(jax.random.fold_in(splits[9], 71), 0),
        "choice_weights": jnp.clip(0.25 + 0.75 * jax.random.uniform(splits[8], (EXPERTS, CAP), jnp.float32) ** level_of(splits[8], (EXPERTS, CAP), ((1, 8),), -0.2, 0.2), 0.25, 1.0),
    }


def reference(tokens, gate_proj, up_proj, down_proj, side_input_weight, dense_out, dense_gate, chosen_rows, choice_weights):
    token_id = ((jnp.arange(CAP) // SLOT) * TOK_DEV).astype(jnp.int32)[None, :] + chosen_rows.astype(jnp.int32)

    def one_expert(routed, inputs):
        w_gate, w_up, w_down, ids, weights = inputs
        picked = jnp.take(tokens, ids, axis=0)
        gate_val = jnp.dot(picked, w_gate, preferred_element_type=jnp.float32)
        up_val = jnp.dot(picked, w_up, preferred_element_type=jnp.float32)
        hidden = (jax.nn.silu(gate_val) * up_val).astype(jnp.bfloat16)
        block_list = hidden.reshape(CAP, N_TP, FF // N_TP).astype(jnp.float32)
        down_weight_blocks = w_down.reshape(N_TP, FF // N_TP, D).astype(jnp.float32)
        part = jnp.einsum('lyk,yka->yla', block_list, down_weight_blocks, precision=lax.Precision.HIGHEST)
        part = lax.optimization_barrier(part.astype(jnp.bfloat16)).astype(jnp.float32)
        expert_out = jnp.sum(part, axis=0).astype(jnp.bfloat16)
        routed = routed.at[ids].add(weights[:, None] * expert_out.astype(jnp.float32))
        return routed, None

    routed, _ = lax.scan(one_expert, jnp.zeros((TOKENS, D), jnp.float32),
                         (gate_proj, up_proj, down_proj, token_id, choice_weights))
    dense_hidden = jax.nn.silu(jnp.dot(tokens, side_input_weight, preferred_element_type=jnp.float32)).astype(jnp.bfloat16)
    dense_val = jnp.dot(dense_hidden, dense_out, preferred_element_type=jnp.float32)
    side_gate = jax.nn.sigmoid(jnp.dot(tokens, dense_gate, preferred_element_type=jnp.float32))
    return (routed + side_gate[:, None] * dense_val).astype(jnp.bfloat16)
```

```python
import functools

import jax
import jax.numpy as jnp
from jax import lax
from jax.experimental import pallas as pl
from jax.experimental.pallas import tpu as pltpu
from jax.sharding import PartitionSpec as P

MESH = pl.DeviceIdType.MESH
LANES = 128


def plain_per_device(
    tokens,
    gate_proj,
    up_proj,
    down_proj,
    side_input_weight,
    dense_out,
    dense_gate,
    chosen_rows,
    choice_weights,
):
    tok_rows = tokens.shape[0]
    width = tokens.shape[1] // lax.axis_size("tp")
    column_position = lax.axis_index("tp") * width
    own_cols = lax.dynamic_slice_in_dim(tokens, column_position, width, 1)
    expert_count, slot_rows = chosen_rows.shape
    capacity = expert_count * slot_rows
    picked = jnp.take(own_cols, chosen_rows.reshape(-1), axis=0).reshape(
        expert_count, slot_rows, width
    )
    arrived = lax.all_to_all(picked, "ep", split_axis=0, concat_axis=1, tiled=True).reshape(
        capacity, width
    )
    piece = lax.all_gather(arrived, "tp", axis=1, tiled=True)
    gate_val = jnp.dot(piece, gate_proj[0], preferred_element_type=jnp.float32)
    up_val = jnp.dot(piece, up_proj[0], preferred_element_type=jnp.float32)
    hidden = (jax.nn.silu(gate_val) * up_val).astype(jnp.bfloat16)
    summed = lax.psum_scatter(
        lax.dot_general(
            down_proj[0], hidden, (((0,), (1,)), ((), ())), preferred_element_type=jnp.float32
        ).astype(jnp.bfloat16),
        "tp",
        scatter_dimension=0,
        tiled=True,
    )
    returned = lax.all_to_all(summed, "ep", split_axis=1, concat_axis=1, tiled=True)
    hits = (
        chosen_rows.reshape(-1)[:, None] == jnp.arange(tok_rows, dtype=jnp.int32)[None, :]
    ).astype(jnp.bfloat16)
    scaled = returned.astype(jnp.float32) * choice_weights.reshape(-1)[None, :]
    high_part = scaled.astype(jnp.bfloat16)
    lower_half = (scaled - high_part.astype(jnp.float32)).astype(jnp.bfloat16)
    contract = (((0,), (1,)), ((), ()))
    routed = lax.dot_general(
        hits, high_part, contract, preferred_element_type=jnp.float32
    ) + lax.dot_general(hits, lower_half, contract, preferred_element_type=jnp.float32)
    dense_hidden = jax.nn.silu(
        jnp.dot(tokens, side_input_weight, preferred_element_type=jnp.float32)
    ).astype(jnp.bfloat16)
    dense_val = jnp.dot(
        lax.all_gather(dense_hidden, "tp", axis=1, tiled=True),
        dense_out,
        preferred_element_type=jnp.float32,
    )
    side_gate = jax.nn.sigmoid(jnp.dot(tokens, dense_gate, preferred_element_type=jnp.float32))
    return (routed + side_gate[:, None] * dense_val).astype(jnp.bfloat16)


def dot(a, b):
    return jnp.dot(a, b, preferred_element_type=jnp.float32)


def silu(v):
    return v / (1.0 + jnp.exp(-v))


def layer_kernel(
    n_ep,
    slot,
    tok_hbm,
    gate_hbm,
    up_hbm,
    down_hbm,
    side_hbm,
    dout_hbm,
    dgate_ref,
    rows_ref,
    cw_ref,
    out_ref,
    tok,
    w_gate,
    w_up,
    w_down,
    w_side,
    w_dout,
    pick,
    xin,
    g_acc,
    u_acc,
    hid,
    comb,
    dhid,
    part,
    d_in,
    rx,
    ry,
    pair,
    fin,
    back,
    load_sem,
    send_sem,
    z_sem,
    ag_sem,
    dh_sem,
    rsd_sem,
    rsx_sem,
    rsy_sem,
    ret_sem,
):
    e = lax.axis_index("ep")
    p = lax.axis_index("tp")
    px = p + 1 - 2 * (p % 2)
    py = p + 2 - 4 * (p // 2)
    pd = px + 2 - 4 * (px // 2)
    z = e // 2
    nz = n_ep // 2
    width = xin.shape[2]
    tok_rows = tok.shape[0]
    side = w_side.shape[1]
    to_x, to_y = {"tp": px}, {"tp": py}

    loads = []
    for i, (src, dst) in enumerate(
        (
            (tok_hbm, tok),
            (side_hbm, w_side),
            (gate_hbm.at[0], w_gate),
            (up_hbm.at[0], w_up),
            (down_hbm.at[0], w_down),
            (dout_hbm, w_dout),
        )
    ):
        copy = pltpu.make_async_copy(src, dst, load_sem.at[i])
        copy.start()
        loads.append(copy)

    barrier = pltpu.get_barrier_semaphore()
    for k in range(1, n_ep):
        pl.semaphore_signal(
            barrier, inc=1, device_id={"ep": (e + k) % n_ep}, device_id_type=MESH
        )
    for there in (to_x, to_y):
        pl.semaphore_signal(barrier, inc=1, device_id=there, device_id_type=MESH)

    def block(owner):
        return pl.ds(pl.multiple_of(owner * slot, slot), slot)

    sends = []

    def send(src, dst, sem, there):
        copy = pltpu.make_async_remote_copy(
            src_ref=src,
            dst_ref=dst,
            send_sem=send_sem.at[len(sends)],
            recv_sem=sem,
            device_id=there,
            device_id_type=MESH,
        )
        copy.start()
        sends.append(copy)

    def arrive(dst, sem):
        pltpu.make_async_remote_copy(
            src_ref=dst,
            dst_ref=dst,
            send_sem=send_sem.at[0],
            recv_sem=sem,
            device_id=to_x,
            device_id_type=MESH,
        ).wait_recv()

    rows_t = rows_ref[...].astype(jnp.float32).T
    cw_t = cw_ref[...].T
    lane = lax.broadcasted_iota(jnp.int32, (slot, tok_rows), 1).astype(jnp.float32)
    hits = jnp.concatenate(
        [jnp.where(rows_t[:, k : k + 1] == lane, 1.0, 0.0) for k in range(n_ep)], axis=0
    )
    loads[0].wait()
    own = pl.ds(pl.multiple_of(p * width, width), width)
    pick[...] = dot(hits.astype(jnp.bfloat16), tok[:, own]).astype(jnp.bfloat16)
    pl.semaphore_wait(barrier, n_ep + 1)

    far = sorted(range(1, n_ep), key=lambda k: -min(k, n_ep - k))
    for k in far:
        peer = (e + k) % n_ep
        send(pick.at[block(peer)], xin.at[p, block(e)], z_sem.at[e], {"ep": peer})
    xin[p, block(e)] = pick[block(e), :]

    def spread(owner):
        ref = xin.at[p, block(owner)]
        send(ref, ref, ag_sem.at[0, owner], to_x)
        send(ref, ref, ag_sem.at[1, owner], to_y)

    spread(e)

    loads[1].wait()
    dhid[p] = silu(dot(tok[...], w_side[...])).astype(jnp.bfloat16)
    send(dhid.at[p], dhid.at[p], dh_sem.at[0], to_x)
    send(dhid.at[p], dhid.at[p], dh_sem.at[1], to_y)

    weight = jnp.concatenate([cw_t[:, k : k + 1] for k in range(n_ep)], axis=0)
    both = (hits * weight).T
    high = both.astype(jnp.bfloat16)
    comb[0] = high
    comb[1] = (both - high.astype(jnp.float32)).astype(jnp.bfloat16)

    near = [n_ep - k for k in far[::-1]]
    near = sorted(range(1, n_ep), key=lambda k: min(k, n_ep - k))
    for k in near:
        owner = (e + n_ep - k) % n_ep
        arrive(xin.at[p, block(owner)], z_sem.at[owner])
        spread(owner)

    tile = 2 * LANES
    n_tiles = g_acc.shape[1] // tile

    loads[2].wait()
    loads[3].wait()

    def gate_up(q, first):
        rows = pl.ds(pl.multiple_of(q * width, width), width)

        @pl.loop(0, n_tiles)
        def _(n):
            cols = pl.ds(pl.multiple_of(n * tile, tile), tile)
            g = dot(xin[q], w_gate[rows, cols])
            u = dot(xin[q], w_up[rows, cols])
            if first:
                g_acc[:, cols] = g
                u_acc[:, cols] = u
            else:
                g_acc[:, cols] += g
                u_acc[:, cols] += u

    gate_up(p, True)

    order = [0] + near
    zs = [j for j in range(nz)]
    for j in zs:
        zo = (z + j) % nz
        even, odd = 2 * zo, 2 * zo + 1
        ref = xin.at[px, block(even)]
        arrive(ref, ag_sem.at[0, even])
        send(ref, ref, ag_sem.at[2, even], to_y)
        ref = xin.at[py, block(odd)]
        arrive(ref, ag_sem.at[1, odd])
        send(ref, ref, ag_sem.at[2, odd], to_x)
    half = tok_rows // 2
    arrive(dhid.at[px], dh_sem.at[0])
    ref = dhid.at[px, pl.ds(0, half)]
    send(ref, ref, dh_sem.at[2], to_y)
    arrive(dhid.at[py], dh_sem.at[1])
    ref = dhid.at[py, pl.ds(half, half)]
    send(ref, ref, dh_sem.at[3], to_x)

    for j in zs:
        odd = 2 * j + 1
        arrive(xin.at[px, block(odd)], ag_sem.at[0, odd])
    gate_up(px, False)
    for j in zs:
        even = 2 * j
        arrive(xin.at[py, block(even)], ag_sem.at[1, even])
    gate_up(py, False)
    for owner in range(n_ep):
        arrive(xin.at[pd, block(owner)], ag_sem.at[2, owner])

    last = pl.ds(pl.multiple_of(pd * width, width), width)

    @pl.loop(0, n_tiles)
    def _(n):
        cols = pl.ds(pl.multiple_of(n * tile, tile), tile)
        g = g_acc[:, cols] + dot(xin[pd], w_gate[last, cols])
        u = u_acc[:, cols] + dot(xin[pd], w_up[last, cols])
        hid[:, cols] = (silu(g) * u).astype(jnp.bfloat16)

    loads[4].wait()

    def down(at, q):
        @pl.loop(0, width // tile)
        def _(n):
            cols = pl.ds(pl.multiple_of(n * tile, tile), tile)
            src = pl.ds(pl.multiple_of(q * width + n * tile, tile), tile)
            part[at, :, cols] = dot(hid[...], w_down[:, src]).astype(jnp.bfloat16)

    offs = sorted(range(nz), key=lambda j: (-min(j, nz - j), j))

    def pieces(g):
        zo = (z + offs[g]) % nz
        return 2 * zo, 2 * zo + 1

    def first_d(g):
        even, odd = pieces(g)
        send(part.at[3, block(odd)], d_in.at[block(odd)], rsd_sem.at[odd], to_x)
        send(part.at[3, block(even)], d_in.at[block(even)], rsd_sem.at[even], to_y)

    def direct_x(g):
        odd = pieces(g)[1]
        send(part.at[1, block(odd)], rx.at[block(odd)], rsx_sem.at[odd], to_x)

    def direct_y(g):
        even = pieces(g)[0]
        send(part.at[2, block(even)], ry.at[block(even)], rsy_sem.at[even], to_y)

    def direct(g):
        first_d(g)
        direct_x(g)
        direct_y(g)

    f32 = jnp.float32

    def joined(g):
        even, odd = pieces(g)
        for owner, at, dst, sem, there in (
            (even, 1, rx, rsx_sem, to_x),
            (odd, 2, ry, rsy_sem, to_y),
        ):
            b = block(owner)
            arrive(d_in.at[b], rsd_sem.at[owner])
            pair[b, :] = (part[at, b, :].astype(f32) + d_in[b, :].astype(f32)).astype(
                jnp.bfloat16
            )
            send(pair.at[b], dst.at[b], sem.at[owner], there)

    def finish(g):
        even, odd = pieces(g)
        for owner in (even, odd):
            b = block(owner)
            arrive(rx.at[b], rsx_sem.at[owner])
            arrive(ry.at[b], rsy_sem.at[owner])
            fin[b, :] = (
                part[0, b, :].astype(f32) + rx[b, :].astype(f32) + ry[b, :].astype(f32)
            ).astype(jnp.bfloat16)
            if offs[g]:
                send(fin.at[b], back.at[block(e)], ret_sem.at[e], {"ep": owner})
        if not offs[g]:
            other = e + 1 - 2 * (e % 2)
            send(fin.at[block(other)], back.at[block(e)], ret_sem.at[e], {"ep": other})
            back[block(e), :] = fin[block(e), :]

    down(3, pd)
    first_d(0)
    down(1, px)
    direct_x(0)
    down(2, py)
    direct_y(0)
    if nz > 1:
        direct(1)
    down(0, p)

    for g in range(nz):
        joined(g)
        if g + 2 < nz:
            direct(g + 2)
        if g >= 1:
            finish(g - 1)
        if g == min(1, nz - 1):
            arrive(dhid.at[pd, pl.ds(0, half)], dh_sem.at[2])
            arrive(dhid.at[pd, pl.ds(half, half)], dh_sem.at[3])
            loads[5].wait()
            total = dot(dhid[0], w_dout[pl.ds(0, side)])
            for q in range(1, dhid.shape[0]):
                total += dot(dhid[q], w_dout[pl.ds(q * side, side)])
            logit = jnp.sum(
                tok[...].astype(f32) * dgate_ref[...].astype(f32), axis=1, keepdims=True
            )
            g_acc[:, pl.ds(0, width)] = total / (1.0 + jnp.exp(-logit))
    finish(nz - 1)

    for k in near:
        owner = (e + n_ep - k) % n_ep
        arrive(back.at[block(owner)], ret_sem.at[owner])
    out_ref[...] = (
        g_acc[:, pl.ds(0, width)] + dot(comb[0], back[...]) + dot(comb[1], back[...])
    ).astype(jnp.bfloat16)
    for copy in sends:
        copy.wait_send()


def fused_per_device(
    tokens,
    gate_proj,
    up_proj,
    down_proj,
    side_input_weight,
    dense_out,
    dense_gate,
    chosen_rows,
    choice_weights,
):
    n_ep, slot = chosen_rows.shape
    n_tp = lax.axis_size("tp")
    tok_rows, d = tokens.shape
    width = d // n_tp
    ff = gate_proj.shape[2]
    side = side_input_weight.shape[1]
    cap = n_ep * slot
    bf16, f32 = jnp.bfloat16, jnp.float32
    n_sends = 2 * (n_ep - 1) + 2 * n_ep + n_ep + 4 + 3 * n_ep
    hbm = pl.BlockSpec(memory_space=pltpu.HBM)
    vmem = pl.BlockSpec(memory_space=pltpu.VMEM)
    return pl.pallas_call(
        functools.partial(layer_kernel, n_ep, slot),
        out_shape=jax.ShapeDtypeStruct((tok_rows, width), bf16),
        in_specs=[hbm] * 6 + [vmem] * 3,
        out_specs=vmem,
        scratch_shapes=[
            pltpu.VMEM((tok_rows, d), bf16),
            pltpu.VMEM((d, ff), bf16),
            pltpu.VMEM((d, ff), bf16),
            pltpu.VMEM((ff, d), bf16),
            pltpu.VMEM((d, side), bf16),
            pltpu.VMEM((n_tp * side, width), bf16),
            pltpu.VMEM((cap, width), bf16),
            pltpu.VMEM((n_tp, cap, width), bf16),
            pltpu.VMEM((cap, ff), f32),
            pltpu.VMEM((cap, ff), f32),
            pltpu.VMEM((cap, ff), bf16),
            pltpu.VMEM((2, tok_rows, cap), bf16),
            pltpu.VMEM((n_tp, tok_rows, side), bf16),
            pltpu.VMEM((4, cap, width), bf16),
            pltpu.VMEM((cap, width), bf16),
            pltpu.VMEM((cap, width), bf16),
            pltpu.VMEM((cap, width), bf16),
            pltpu.VMEM((cap, width), bf16),
            pltpu.VMEM((cap, width), bf16),
            pltpu.VMEM((cap, width), bf16),
            pltpu.SemaphoreType.DMA((6,)),
            pltpu.SemaphoreType.DMA((n_sends,)),
            pltpu.SemaphoreType.DMA((n_ep,)),
            pltpu.SemaphoreType.DMA((3, n_ep)),
            pltpu.SemaphoreType.DMA((4,)),
            pltpu.SemaphoreType.DMA((n_ep,)),
            pltpu.SemaphoreType.DMA((n_ep,)),
            pltpu.SemaphoreType.DMA((n_ep,)),
            pltpu.SemaphoreType.DMA((n_ep,)),
        ],
        compiler_params=pltpu.CompilerParams(collective_id=0, has_side_effects=True),
    )(
        tokens,
        gate_proj,
        up_proj,
        down_proj,
        side_input_weight,
        dense_out,
        dense_gate.reshape(1, d),
        chosen_rows,
        choice_weights,
    )


def per_device(*args):
    tokens, gate_proj, chosen_rows = args[0], args[1], args[7]
    n_ep, slot = chosen_rows.shape
    n_tp = lax.axis_size("tp")
    width, tile = tokens.shape[1] // n_tp, 2 * LANES
    fits = (
        n_tp == 4
        and n_ep % 2 == 0
        and tokens.shape[0] == n_ep * slot
        and slot % 16 == 0
        and width % tile == 0
        and gate_proj.shape[2] % tile == 0
        and args[4].shape[1] % LANES == 0
    )
    return fused_per_device(*args) if fits else plain_per_device(*args)


def solution(mesh):
    placed = (
        P("ep", None),
        P("ep", None, "tp"),
        P("ep", None, "tp"),
        P("ep", "tp", None),
        P(None, "tp"),
        P(None, "tp"),
        P(),
        P(None, "ep"),
        P(None, "ep"),
    )
    return jax.shard_map(
        per_device, mesh=mesh, in_specs=placed, out_specs=P("ep", "tp"), check_vma=False
    )
```

```python
import functools

import jax
import jax.numpy as jnp
from jax import lax
from jax.experimental import pallas as pl
from jax.experimental.pallas import tpu as pltpu
from jax.sharding import PartitionSpec as P

MESH = pl.DeviceIdType.MESH
LANES = 128


def plain_per_device(
    tokens,
    gate_proj,
    up_proj,
    down_proj,
    side_input_weight,
    dense_out,
    dense_gate,
    chosen_rows,
    choice_weights,
):
    tok_rows = tokens.shape[0]
    width = tokens.shape[1] // lax.axis_size("tp")
    column_position = lax.axis_index("tp") * width
    own_cols = lax.dynamic_slice_in_dim(tokens, column_position, width, 1)
    expert_count, slot_rows = chosen_rows.shape
    capacity = expert_count * slot_rows
    picked = jnp.take(own_cols, chosen_rows.reshape(-1), axis=0).reshape(
        expert_count, slot_rows, width
    )
    arrived = lax.all_to_all(picked, "ep", split_axis=0, concat_axis=1, tiled=True).reshape(
        capacity, width
    )
    piece = lax.all_gather(arrived, "tp", axis=1, tiled=True)
    gate_val = jnp.dot(piece, gate_proj[0], preferred_element_type=jnp.float32)
    up_val = jnp.dot(piece, up_proj[0], preferred_element_type=jnp.float32)
    hidden = (jax.nn.silu(gate_val) * up_val).astype(jnp.bfloat16)
    summed = lax.psum_scatter(
        lax.dot_general(
            down_proj[0], hidden, (((0,), (1,)), ((), ())), preferred_element_type=jnp.float32
        ).astype(jnp.bfloat16),
        "tp",
        scatter_dimension=0,
        tiled=True,
    )
    returned = lax.all_to_all(summed, "ep", split_axis=1, concat_axis=1, tiled=True)
    hits = (
        chosen_rows.reshape(-1)[:, None] == jnp.arange(tok_rows, dtype=jnp.int32)[None, :]
    ).astype(jnp.bfloat16)
    scaled = returned.astype(jnp.float32) * choice_weights.reshape(-1)[None, :]
    high_part = scaled.astype(jnp.bfloat16)
    lower_half = (scaled - high_part.astype(jnp.float32)).astype(jnp.bfloat16)
    contract = (((0,), (1,)), ((), ()))
    routed = lax.dot_general(
        hits, high_part, contract, preferred_element_type=jnp.float32
    ) + lax.dot_general(hits, lower_half, contract, preferred_element_type=jnp.float32)
    dense_hidden = jax.nn.silu(
        jnp.dot(tokens, side_input_weight, preferred_element_type=jnp.float32)
    ).astype(jnp.bfloat16)
    dense_val = jnp.dot(
        lax.all_gather(dense_hidden, "tp", axis=1, tiled=True),
        dense_out,
        preferred_element_type=jnp.float32,
    )
    side_gate = jax.nn.sigmoid(jnp.dot(tokens, dense_gate, preferred_element_type=jnp.float32))
    return (routed + side_gate[:, None] * dense_val).astype(jnp.bfloat16)


def dot(a, b):
    return jnp.dot(a, b, preferred_element_type=jnp.float32)


def silu(v):
    return v / (1.0 + jnp.exp(-v))


def layer_kernel(
    n_ep,
    slot,
    tok_hbm,
    gate_hbm,
    up_hbm,
    down_hbm,
    side_hbm,
    dout_hbm,
    dgate_ref,
    rows_ref,
    cw_ref,
    out_ref,
    tok,
    w_gate,
    w_up,
    w_down,
    w_side,
    w_dout,
    pick,
    xin,
    g_acc,
    u_acc,
    hid,
    comb,
    dhid,
    part,
    d_in,
    rx,
    ry,
    pair,
    fin,
    back,
    load_sem,
    send_sem,
    z_sem,
    ag_sem,
    dh_sem,
    rsd_sem,
    rsx_sem,
    rsy_sem,
    ret_sem,
):
    e = lax.axis_index("ep")
    p = lax.axis_index("tp")
    px = p + 1 - 2 * (p % 2)
    py = p + 2 - 4 * (p // 2)
    pd = px + 2 - 4 * (px // 2)
    z = e // 2
    nz = n_ep // 2
    width = xin.shape[2]
    tok_rows = tok.shape[0]
    side = w_side.shape[1]
    to_x, to_y = {"tp": px}, {"tp": py}

    loads = []
    for i, (src, dst) in enumerate(
        (
            (tok_hbm, tok),
            (side_hbm, w_side),
            (gate_hbm.at[0], w_gate),
            (up_hbm.at[0], w_up),
            (down_hbm.at[0], w_down),
            (dout_hbm, w_dout),
        )
    ):
        copy = pltpu.make_async_copy(src, dst, load_sem.at[i])
        copy.start()
        loads.append(copy)

    barrier = pltpu.get_barrier_semaphore()
    for k in range(1, n_ep):
        pl.semaphore_signal(
            barrier, inc=1, device_id={"ep": (e + k) % n_ep}, device_id_type=MESH
        )
    for there in (to_x, to_y):
        pl.semaphore_signal(barrier, inc=1, device_id=there, device_id_type=MESH)

    def block(owner):
        return pl.ds(pl.multiple_of(owner * slot, slot), slot)

    sends = []

    def send(src, dst, sem, there):
        copy = pltpu.make_async_remote_copy(
            src_ref=src,
            dst_ref=dst,
            send_sem=send_sem.at[len(sends)],
            recv_sem=sem,
            device_id=there,
            device_id_type=MESH,
        )
        copy.start()
        sends.append(copy)

    def arrive(dst, sem):
        pltpu.make_async_remote_copy(
            src_ref=dst,
            dst_ref=dst,
            send_sem=send_sem.at[0],
            recv_sem=sem,
            device_id=to_x,
            device_id_type=MESH,
        ).wait_recv()

    rows_t = rows_ref[...].astype(jnp.float32).T
    cw_t = cw_ref[...].T
    lane = lax.broadcasted_iota(jnp.int32, (slot, tok_rows), 1).astype(jnp.float32)
    hits = jnp.concatenate(
        [jnp.where(rows_t[:, k : k + 1] == lane, 1.0, 0.0) for k in range(n_ep)], axis=0
    )
    loads[0].wait()
    own = pl.ds(pl.multiple_of(p * width, width), width)
    pick[...] = dot(hits.astype(jnp.bfloat16), tok[:, own]).astype(jnp.bfloat16)
    pl.semaphore_wait(barrier, n_ep + 1)

    if nz == 4:
        upper = z // 2
        inner = (z + upper) % 2
        chips = [z, z + 1 - 2 * (z % 2), 2 - upper, 3 - 3 * upper]
        goals = chips
        places = [0, 1, 3 - inner, 3 - inner]
        turn = [2, 3, 1, 0]
    else:
        chips = [(z + nz - g) % nz for g in range(nz)]
        goals = [(z + g) % nz for g in range(nz)]
        places = list(range(nz))
        turn = [*range(1, nz), 0]
    core = e % 2
    partner = e + 1 - 2 * core

    def at(pos):
        return pl.ds(pl.multiple_of(pos * slot, slot), slot)

    send(pick.at[block(partner)], xin.at[p, at(1)], z_sem.at[1], {"ep": partner})
    for g in range(1, nz):
        for c in range(2):
            peer = 2 * goals[g] + c
            mine = 2 * places[g] + core
            send(pick.at[block(peer)], xin.at[p, at(mine)], z_sem.at[mine], {"ep": peer})
    xin[p, at(0)] = pick[block(e), :]

    def spread(pos):
        ref = xin.at[p, at(pos)]
        send(ref, ref, ag_sem.at[0, pos], to_x)
        send(ref, ref, ag_sem.at[1, pos], to_y)

    def forward(pos):
        if pos % 2 == 0:
            ref = xin.at[px, at(pos)]
            arrive(ref, ag_sem.at[0, pos])
            send(ref, ref, ag_sem.at[2, pos], to_y)
        else:
            ref = xin.at[py, at(pos)]
            arrive(ref, ag_sem.at[1, pos])
            send(ref, ref, ag_sem.at[2, pos], to_x)

    spread(0)
    loads[1].wait()
    dhid[p] = silu(dot(tok[...], w_side[...])).astype(jnp.bfloat16)
    arrive(xin.at[p, at(1)], z_sem.at[1])
    spread(1)
    send(dhid.at[p], dhid.at[p], dh_sem.at[0], to_x)
    send(dhid.at[p], dhid.at[p], dh_sem.at[1], to_y)

    weight = jnp.concatenate([cw_t[:, k : k + 1] for k in range(n_ep)], axis=0)
    both = (hits * weight).T
    high = both.astype(jnp.bfloat16)
    comb[0] = high
    comb[1] = (both - high.astype(jnp.float32)).astype(jnp.bfloat16)

    tile = 2 * LANES
    n_tiles = g_acc.shape[1] // tile
    f32 = jnp.float32
    half = tok_rows // 2

    def gate_up(q, first):
        rows = pl.ds(pl.multiple_of(q * width, width), width)

        @pl.loop(0, n_tiles)
        def _(n):
            cols = pl.ds(pl.multiple_of(n * tile, tile), tile)
            g = dot(xin[q], w_gate[rows, cols])
            u = dot(xin[q], w_up[rows, cols])
            if first:
                g_acc[:, cols] = g
                u_acc[:, cols] = u
            else:
                g_acc[:, cols] += g
                u_acc[:, cols] += u

    def gate_up_last(q):
        rows = pl.ds(pl.multiple_of(q * width, width), width)

        @pl.loop(0, n_tiles)
        def _(n):
            cols = pl.ds(pl.multiple_of(n * tile, tile), tile)
            g = g_acc[:, cols] + dot(xin[q], w_gate[rows, cols])
            u = u_acc[:, cols] + dot(xin[q], w_up[rows, cols])
            hid[:, cols] = (silu(g) * u).astype(jnp.bfloat16)

    def down(to, q):

        @pl.loop(0, width // tile)
        def _(n):
            cols = pl.ds(pl.multiple_of(n * tile, tile), tile)
            src = pl.ds(pl.multiple_of(q * width + n * tile, tile), tile)
            part[to, :, cols] = dot(hid[...], w_down[:, src]).astype(jnp.bfloat16)

    def wait_x():
        for pos in range(n_ep):
            if pos % 2:
                arrive(xin.at[px, at(pos)], ag_sem.at[0, pos])

    def wait_y():
        for pos in range(n_ep):
            if pos % 2 == 0:
                arrive(xin.at[py, at(pos)], ag_sem.at[1, pos])

    def wait_d():
        for pos in range(n_ep):
            arrive(xin.at[pd, at(pos)], ag_sem.at[2, pos])

    def first_d(g):
        even, odd = at(2 * g), at(2 * g + 1)
        send(part.at[3, odd], d_in.at[odd], rsd_sem.at[2 * g + 1], to_x)
        send(part.at[3, even], d_in.at[even], rsd_sem.at[2 * g], to_y)

    def direct_x(g):
        odd = at(2 * g + 1)
        send(part.at[1, odd], rx.at[odd], rsx_sem.at[2 * g + 1], to_x)

    def direct_y(g):
        even = at(2 * g)
        send(part.at[2, even], ry.at[even], rsy_sem.at[2 * g], to_y)

    def joined(g):
        for pos, src, dst, sem, there in (
            (2 * g, 1, rx, rsx_sem, to_x),
            (2 * g + 1, 2, ry, rsy_sem, to_y),
        ):
            b = at(pos)
            arrive(d_in.at[b], rsd_sem.at[pos])
            pair[b, :] = (part[src, b, :].astype(f32) + d_in[b, :].astype(f32)).astype(
                jnp.bfloat16
            )
            send(pair.at[b], dst.at[b], sem.at[pos], there)

    def finish(g):
        for c in range(2):
            pos = 2 * g + c
            b = at(pos)
            arrive(rx.at[b], rsx_sem.at[pos])
            arrive(ry.at[b], rsy_sem.at[pos])
            total = (
                part[0, b, :].astype(f32) + rx[b, :].astype(f32) + ry[b, :].astype(f32)
            ).astype(jnp.bfloat16)
            if pos == 0:
                back[block(e), :] = total
            else:
                fin[b, :] = total
                owner = partner if g == 0 else 2 * chips[g] + c
                send(fin.at[b], back.at[block(e)], ret_sem.at[e], {"ep": owner})

    lag = n_ep
    for pos in range(2, n_ep):
        arrive(xin.at[p, at(pos)], z_sem.at[pos])
        spread(pos)
        if pos >= lag:
            forward(pos - lag)
    loads[2].wait()
    loads[3].wait()
    gate_up(p, True)
    for pos in range(n_ep - lag, n_ep):
        forward(pos)
    arrive(dhid.at[px], dh_sem.at[0])
    ref = dhid.at[px, pl.ds(0, half)]
    send(ref, ref, dh_sem.at[2], to_y)
    arrive(dhid.at[py], dh_sem.at[1])
    ref = dhid.at[py, pl.ds(half, half)]
    send(ref, ref, dh_sem.at[3], to_x)
    wait_x()
    gate_up(px, False)
    wait_y()
    gate_up(py, False)
    wait_d()
    gate_up_last(pd)

    loads[4].wait()
    down(3, pd)
    first_d(turn[0])
    first_d(turn[1])
    down(1, px)
    direct_x(turn[0])
    down(2, py)
    direct_y(turn[0])
    direct_x(turn[1])
    direct_y(turn[1])
    down(0, p)
    for i in range(nz):
        joined(turn[i])
        if i + 2 < nz:
            first_d(turn[i + 2])
            direct_x(turn[i + 2])
            direct_y(turn[i + 2])
        if i >= 1:
            finish(turn[i - 1])
        if i == 1:
            arrive(dhid.at[pd, pl.ds(0, half)], dh_sem.at[2])
            arrive(dhid.at[pd, pl.ds(half, half)], dh_sem.at[3])
            loads[5].wait()
            total = dot(dhid[0], w_dout[pl.ds(0, side)])
            for q in range(1, dhid.shape[0]):
                total += dot(dhid[q], w_dout[pl.ds(q * side, side)])
            logit = jnp.sum(
                tok[...].astype(f32) * dgate_ref[...].reshape(1, tok.shape[1]).astype(f32),
                axis=1,
                keepdims=True,
            )
            g_acc[:, pl.ds(0, width)] = total / (1.0 + jnp.exp(-logit))
    finish(turn[-1])

    for k in range(1, n_ep):
        owner = (e + n_ep - k) % n_ep
        arrive(back.at[block(owner)], ret_sem.at[owner])
    out_ref[...] = (
        g_acc[:, pl.ds(0, width)] + dot(comb[0], back[...]) + dot(comb[1], back[...])
    )
    for copy in sends:
        copy.wait_send()


def fused_per_device(
    tokens,
    gate_proj,
    up_proj,
    down_proj,
    side_input_weight,
    dense_out,
    dense_gate,
    chosen_rows,
    choice_weights,
):
    n_ep, slot = chosen_rows.shape
    n_tp = lax.axis_size("tp")
    tok_rows, d = tokens.shape
    width = d // n_tp
    ff = gate_proj.shape[2]
    side = side_input_weight.shape[1]
    cap = n_ep * slot
    bf16, f32 = jnp.bfloat16, jnp.float32
    n_sends = 2 * (n_ep - 1) + 2 * n_ep + n_ep + 4 + 3 * n_ep
    hbm = pl.BlockSpec(memory_space=pltpu.HBM)
    vmem = pl.BlockSpec(memory_space=pltpu.VMEM)
    return pl.pallas_call(
        functools.partial(layer_kernel, n_ep, slot),
        out_shape=pltpu.VMEM((tok_rows, width), f32),
        in_specs=[hbm] * 6 + [vmem] * 3,
        out_specs=vmem,
        scratch_shapes=[
            pltpu.VMEM((tok_rows, d), bf16),
            pltpu.VMEM((d, ff), bf16),
            pltpu.VMEM((d, ff), bf16),
            pltpu.VMEM((ff, d), bf16),
            pltpu.VMEM((d, side), bf16),
            pltpu.VMEM((n_tp * side, width), bf16),
            pltpu.VMEM((cap, width), bf16),
            pltpu.VMEM((n_tp, cap, width), bf16),
            pltpu.VMEM((cap, ff), f32),
            pltpu.VMEM((cap, ff), f32),
            pltpu.VMEM((cap, ff), bf16),
            pltpu.VMEM((2, tok_rows, cap), bf16),
            pltpu.VMEM((n_tp, tok_rows, side), bf16),
            pltpu.VMEM((4, cap, width), bf16),
            pltpu.VMEM((cap, width), bf16),
            pltpu.VMEM((cap, width), bf16),
            pltpu.VMEM((cap, width), bf16),
            pltpu.VMEM((cap, width), bf16),
            pltpu.VMEM((cap, width), bf16),
            pltpu.VMEM((cap, width), bf16),
            pltpu.SemaphoreType.DMA((6,)),
            pltpu.SemaphoreType.DMA((n_sends,)),
            pltpu.SemaphoreType.DMA((n_ep,)),
            pltpu.SemaphoreType.DMA((3, n_ep)),
            pltpu.SemaphoreType.DMA((4,)),
            pltpu.SemaphoreType.DMA((n_ep,)),
            pltpu.SemaphoreType.DMA((n_ep,)),
            pltpu.SemaphoreType.DMA((n_ep,)),
            pltpu.SemaphoreType.DMA((n_ep,)),
        ],
        compiler_params=pltpu.CompilerParams(collective_id=0, has_side_effects=True),
    )(
        tokens,
        gate_proj,
        up_proj,
        down_proj,
        side_input_weight,
        dense_out,
        dense_gate,
        chosen_rows,
        choice_weights,
    ).astype(bf16)


def per_device(*args):
    tokens, gate_proj, chosen_rows = args[0], args[1], args[7]
    n_ep, slot = chosen_rows.shape
    n_tp = lax.axis_size("tp")
    width, tile = tokens.shape[1] // n_tp, 2 * LANES
    fits = (
        n_tp == 4
        and n_ep % 4 == 0
        and tokens.shape[0] == n_ep * slot
        and slot % 16 == 0
        and width % tile == 0
        and gate_proj.shape[2] % tile == 0
        and args[4].shape[1] % LANES == 0
    )
    return fused_per_device(*args) if fits else plain_per_device(*args)


def solution(mesh):
    placed = (
        P("ep", None),
        P("ep", None, "tp"),
        P("ep", None, "tp"),
        P("ep", "tp", None),
        P(None, "tp"),
        P(None, "tp"),
        P(),
        P(None, "ep"),
        P(None, "ep"),
    )
    return jax.shard_map(
        per_device, mesh=mesh, in_specs=placed, out_specs=P("ep", "tp"), check_vma=False
    )
```

```python
import functools

import jax
import jax.numpy as jnp
from jax import lax
from jax.experimental import pallas as pl
from jax.experimental.pallas import tpu as pltpu
from jax.sharding import PartitionSpec as P

MESH = pl.DeviceIdType.MESH
LANES = 128


def plain_per_device(
    tokens,
    gate_proj,
    up_proj,
    down_proj,
    side_input_weight,
    dense_out,
    dense_gate,
    chosen_rows,
    choice_weights,
):
    tok_rows = tokens.shape[0]
    width = tokens.shape[1] // lax.axis_size("tp")
    column_position = lax.axis_index("tp") * width
    own_cols = lax.dynamic_slice_in_dim(tokens, column_position, width, 1)
    expert_count, slot_rows = chosen_rows.shape
    capacity = expert_count * slot_rows
    picked = jnp.take(own_cols, chosen_rows.reshape(-1), axis=0).reshape(
        expert_count, slot_rows, width
    )
    arrived = lax.all_to_all(picked, "ep", split_axis=0, concat_axis=1, tiled=True).reshape(
        capacity, width
    )
    piece = lax.all_gather(arrived, "tp", axis=1, tiled=True)
    gate_val = jnp.dot(piece, gate_proj[0], preferred_element_type=jnp.float32)
    up_val = jnp.dot(piece, up_proj[0], preferred_element_type=jnp.float32)
    hidden = (jax.nn.silu(gate_val) * up_val).astype(jnp.bfloat16)
    summed = lax.psum_scatter(
        lax.dot_general(
            down_proj[0], hidden, (((0,), (1,)), ((), ())), preferred_element_type=jnp.float32
        ).astype(jnp.bfloat16),
        "tp",
        scatter_dimension=0,
        tiled=True,
    )
    returned = lax.all_to_all(summed, "ep", split_axis=1, concat_axis=1, tiled=True)
    hits = (
        chosen_rows.reshape(-1)[:, None] == jnp.arange(tok_rows, dtype=jnp.int32)[None, :]
    ).astype(jnp.bfloat16)
    scaled = returned.astype(jnp.float32) * choice_weights.reshape(-1)[None, :]
    high_part = scaled.astype(jnp.bfloat16)
    lower_half = (scaled - high_part.astype(jnp.float32)).astype(jnp.bfloat16)
    contract = (((0,), (1,)), ((), ()))
    routed = lax.dot_general(
        hits, high_part, contract, preferred_element_type=jnp.float32
    ) + lax.dot_general(hits, lower_half, contract, preferred_element_type=jnp.float32)
    dense_hidden = jax.nn.silu(
        jnp.dot(tokens, side_input_weight, preferred_element_type=jnp.float32)
    ).astype(jnp.bfloat16)
    dense_val = jnp.dot(
        lax.all_gather(dense_hidden, "tp", axis=1, tiled=True),
        dense_out,
        preferred_element_type=jnp.float32,
    )
    side_gate = jax.nn.sigmoid(jnp.dot(tokens, dense_gate, preferred_element_type=jnp.float32))
    return (routed + side_gate[:, None] * dense_val).astype(jnp.bfloat16)


def dot(a, b):
    return jnp.dot(a, b, preferred_element_type=jnp.float32)


def silu(v):
    return v / (1.0 + jnp.exp(-v))


def layer_kernel(
    n_ep,
    slot,
    tok_hbm,
    gate_hbm,
    up_hbm,
    down_hbm,
    side_hbm,
    dout_hbm,
    dgate_ref,
    rows_ref,
    cw_ref,
    out_ref,
    tok,
    w_gate,
    w_up,
    w_down,
    w_side,
    w_dout,
    pick,
    xin,
    g_acc,
    u_acc,
    hid,
    comb,
    dhid,
    part,
    d_in,
    rx,
    ry,
    pair,
    fin,
    back,
    load_sem,
    send_sem,
    z_sem,
    ag_sem,
    dh_sem,
    rsd_sem,
    rsx_sem,
    rsy_sem,
    ret_sem,
):
    e = lax.axis_index("ep")
    p = lax.axis_index("tp")
    px = p + 1 - 2 * (p % 2)
    py = p + 2 - 4 * (p // 2)
    pd = px + 2 - 4 * (px // 2)
    z = e // 2
    nz = n_ep // 2
    width = xin.shape[2]
    tok_rows = tok.shape[0]
    side = w_side.shape[1]
    to_x, to_y = {"tp": px}, {"tp": py}

    loads = []
    for i, (src, dst) in enumerate(
        (
            (tok_hbm, tok),
            (side_hbm, w_side),
            (gate_hbm.at[0], w_gate),
            (up_hbm.at[0], w_up),
            (down_hbm.at[0], w_down),
            (dout_hbm, w_dout),
        )
    ):
        copy = pltpu.make_async_copy(src, dst, load_sem.at[i])
        copy.start()
        loads.append(copy)

    barrier = pltpu.get_barrier_semaphore()
    for k in range(1, n_ep):
        pl.semaphore_signal(
            barrier, inc=1, device_id={"ep": (e + k) % n_ep}, device_id_type=MESH
        )
    for there in (to_x, to_y):
        pl.semaphore_signal(barrier, inc=1, device_id=there, device_id_type=MESH)

    def block(owner):
        return pl.ds(pl.multiple_of(owner * slot, slot), slot)

    sends = []

    def send(src, dst, sem, there):
        copy = pltpu.make_async_remote_copy(
            src_ref=src,
            dst_ref=dst,
            send_sem=send_sem.at[len(sends)],
            recv_sem=sem,
            device_id=there,
            device_id_type=MESH,
        )
        copy.start()
        sends.append(copy)

    def arrive(dst, sem):
        pltpu.make_async_remote_copy(
            src_ref=dst,
            dst_ref=dst,
            send_sem=send_sem.at[0],
            recv_sem=sem,
            device_id=to_x,
            device_id_type=MESH,
        ).wait_recv()

    rows_t = rows_ref[...].astype(jnp.float32).T
    cw_t = cw_ref[...].T
    lane = lax.broadcasted_iota(jnp.int32, (slot, tok_rows), 1).astype(jnp.float32)
    hits = jnp.concatenate(
        [jnp.where(rows_t[:, k : k + 1] == lane, 1.0, 0.0) for k in range(n_ep)], axis=0
    )
    loads[0].wait()
    own = pl.ds(pl.multiple_of(p * width, width), width)
    pick[...] = dot(hits.astype(jnp.bfloat16), tok[:, own]).astype(jnp.bfloat16)
    pl.semaphore_wait(barrier, n_ep + 1)

    if nz == 4:
        upper = z // 2
        inner = (z + upper) % 2
        chips = [z, z + 1 - 2 * (z % 2), 2 - upper, 3 - 3 * upper]
        goals = chips
        places = [0, 1, 3 - inner, 3 - inner]
        turn = [2, 3, 1, 0]
    else:
        chips = [(z + nz - g) % nz for g in range(nz)]
        goals = [(z + g) % nz for g in range(nz)]
        places = list(range(nz))
        turn = [*range(1, nz), 0]
    core = e % 2
    partner = e + 1 - 2 * core

    def at(pos):
        return pl.ds(pl.multiple_of(pos * slot, slot), slot)

    send(pick.at[block(partner)], xin.at[p, at(1)], z_sem.at[1], {"ep": partner})
    for g in range(1, nz):
        for c in range(2):
            peer = 2 * goals[g] + c
            mine = 2 * places[g] + core
            send(pick.at[block(peer)], xin.at[p, at(mine)], z_sem.at[mine], {"ep": peer})
    xin[p, at(0)] = pick[block(e), :]

    def spread(pos):
        ref = xin.at[p, at(pos)]
        send(ref, ref, ag_sem.at[0, pos], to_x)
        send(ref, ref, ag_sem.at[1, pos], to_y)

    def forward(pos):
        if pos % 2 == 0:
            ref = xin.at[px, at(pos)]
            arrive(ref, ag_sem.at[0, pos])
            send(ref, ref, ag_sem.at[2, pos], to_y)
        else:
            ref = xin.at[py, at(pos)]
            arrive(ref, ag_sem.at[1, pos])
            send(ref, ref, ag_sem.at[2, pos], to_x)

    spread(0)
    loads[1].wait()
    dhid[p] = silu(dot(tok[...], w_side[...])).astype(jnp.bfloat16)
    arrive(xin.at[p, at(1)], z_sem.at[1])
    spread(1)
    send(dhid.at[p], dhid.at[p], dh_sem.at[0], to_x)
    send(dhid.at[p], dhid.at[p], dh_sem.at[1], to_y)

    weight = jnp.concatenate([cw_t[:, k : k + 1] for k in range(n_ep)], axis=0)
    both = (hits * weight).T
    high = both.astype(jnp.bfloat16)
    comb[0] = high
    comb[1] = (both - high.astype(jnp.float32)).astype(jnp.bfloat16)

    tile = 2 * LANES
    n_tiles = g_acc.shape[1] // tile
    f32 = jnp.float32
    half = tok_rows // 2

    def gate_up(q, first):
        rows = pl.ds(pl.multiple_of(q * width, width), width)

        @pl.loop(0, n_tiles)
        def _(n):
            cols = pl.ds(pl.multiple_of(n * tile, tile), tile)
            g = dot(xin[q], w_gate[rows, cols])
            u = dot(xin[q], w_up[rows, cols])
            if first:
                g_acc[:, cols] = g
                u_acc[:, cols] = u
            else:
                g_acc[:, cols] += g
                u_acc[:, cols] += u

    def gate_up_last(q):
        rows = pl.ds(pl.multiple_of(q * width, width), width)

        @pl.loop(0, n_tiles)
        def _(n):
            cols = pl.ds(pl.multiple_of(n * tile, tile), tile)
            g = g_acc[:, cols] + dot(xin[q], w_gate[rows, cols])
            u = u_acc[:, cols] + dot(xin[q], w_up[rows, cols])
            hid[:, cols] = (silu(g) * u).astype(jnp.bfloat16)

    def down(to, q):

        @pl.loop(0, width // tile)
        def _(n):
            cols = pl.ds(pl.multiple_of(n * tile, tile), tile)
            src = pl.ds(pl.multiple_of(q * width + n * tile, tile), tile)
            part[to, :, cols] = dot(hid[...], w_down[:, src]).astype(jnp.bfloat16)

    def wait_x():
        for pos in range(n_ep):
            if pos % 2:
                arrive(xin.at[px, at(pos)], ag_sem.at[0, pos])

    def wait_y():
        for pos in range(n_ep):
            if pos % 2 == 0:
                arrive(xin.at[py, at(pos)], ag_sem.at[1, pos])

    def wait_d():
        for pos in range(n_ep):
            arrive(xin.at[pd, at(pos)], ag_sem.at[2, pos])

    def first_d(g):
        even, odd = at(2 * g), at(2 * g + 1)
        send(part.at[3, odd], d_in.at[odd], rsd_sem.at[2 * g + 1], to_x)
        send(part.at[3, even], d_in.at[even], rsd_sem.at[2 * g], to_y)

    def direct_x(g):
        odd = at(2 * g + 1)
        send(part.at[1, odd], rx.at[odd], rsx_sem.at[2 * g + 1], to_x)

    def direct_y(g):
        even = at(2 * g)
        send(part.at[2, even], ry.at[even], rsy_sem.at[2 * g], to_y)

    def joined(g):
        for pos, src, dst, sem, there in (
            (2 * g, 1, rx, rsx_sem, to_x),
            (2 * g + 1, 2, ry, rsy_sem, to_y),
        ):
            b = at(pos)
            arrive(d_in.at[b], rsd_sem.at[pos])
            pair[b, :] = (part[src, b, :].astype(f32) + d_in[b, :].astype(f32)).astype(
                jnp.bfloat16
            )
            send(pair.at[b], dst.at[b], sem.at[pos], there)

    def finish(g):
        for c in range(2):
            pos = 2 * g + c
            b = at(pos)
            arrive(rx.at[b], rsx_sem.at[pos])
            arrive(ry.at[b], rsy_sem.at[pos])
            total = (
                part[0, b, :].astype(f32) + rx[b, :].astype(f32) + ry[b, :].astype(f32)
            ).astype(jnp.bfloat16)
            if pos == 0:
                back[block(e), :] = total
            else:
                fin[b, :] = total
                owner = partner if g == 0 else 2 * chips[g] + c
                send(fin.at[b], back.at[block(e)], ret_sem.at[e], {"ep": owner})

    lag = n_ep
    for pos in range(2, n_ep):
        arrive(xin.at[p, at(pos)], z_sem.at[pos])
        spread(pos)
        if pos >= lag:
            forward(pos - lag)
    loads[2].wait()
    loads[3].wait()
    gate_up(p, True)
    for pos in range(n_ep - lag, n_ep):
        forward(pos)
    arrive(dhid.at[px], dh_sem.at[0])
    ref = dhid.at[px, pl.ds(0, half)]
    send(ref, ref, dh_sem.at[2], to_y)
    arrive(dhid.at[py], dh_sem.at[1])
    ref = dhid.at[py, pl.ds(half, half)]
    send(ref, ref, dh_sem.at[3], to_x)
    wait_x()
    gate_up(px, False)
    wait_y()
    gate_up(py, False)
    wait_d()
    gate_up_last(pd)

    loads[4].wait()
    down(3, pd)
    first_d(turn[0])
    first_d(turn[1])
    down(1, px)
    direct_x(turn[0])
    down(2, py)
    direct_y(turn[0])
    direct_x(turn[1])
    direct_y(turn[1])
    down(0, p)
    for i in range(nz):
        joined(turn[i])
        if i + 2 < nz:
            first_d(turn[i + 2])
            direct_x(turn[i + 2])
            direct_y(turn[i + 2])
        if i >= 2:
            finish(turn[i - 2])
        if i == 1:
            arrive(dhid.at[pd, pl.ds(0, half)], dh_sem.at[2])
            arrive(dhid.at[pd, pl.ds(half, half)], dh_sem.at[3])
            loads[5].wait()
            total = dot(dhid[0], w_dout[pl.ds(0, side)])
            for q in range(1, dhid.shape[0]):
                total += dot(dhid[q], w_dout[pl.ds(q * side, side)])
            logit = jnp.sum(
                tok[...].astype(f32) * dgate_ref[...].reshape(1, tok.shape[1]).astype(f32),
                axis=1,
                keepdims=True,
            )
            g_acc[:, pl.ds(0, width)] = total / (1.0 + jnp.exp(-logit))
    finish(turn[-2])
    finish(turn[-1])

    for k in range(1, n_ep):
        owner = (e + n_ep - k) % n_ep
        arrive(back.at[block(owner)], ret_sem.at[owner])
    out_ref[...] = (
        g_acc[:, pl.ds(0, width)] + dot(comb[0], back[...]) + dot(comb[1], back[...])
    )
    for copy in sends:
        copy.wait_send()


def fused_per_device(
    tokens,
    gate_proj,
    up_proj,
    down_proj,
    side_input_weight,
    dense_out,
    dense_gate,
    chosen_rows,
    choice_weights,
):
    n_ep, slot = chosen_rows.shape
    n_tp = lax.axis_size("tp")
    tok_rows, d = tokens.shape
    width = d // n_tp
    ff = gate_proj.shape[2]
    side = side_input_weight.shape[1]
    cap = n_ep * slot
    bf16, f32 = jnp.bfloat16, jnp.float32
    n_sends = 2 * (n_ep - 1) + 2 * n_ep + n_ep + 4 + 3 * n_ep
    hbm = pl.BlockSpec(memory_space=pltpu.HBM)
    vmem = pl.BlockSpec(memory_space=pltpu.VMEM)
    return pl.pallas_call(
        functools.partial(layer_kernel, n_ep, slot),
        out_shape=pltpu.VMEM((tok_rows, width), f32),
        in_specs=[hbm] * 6 + [vmem] * 3,
        out_specs=vmem,
        scratch_shapes=[
            pltpu.VMEM((tok_rows, d), bf16),
            pltpu.VMEM((d, ff), bf16),
            pltpu.VMEM((d, ff), bf16),
            pltpu.VMEM((ff, d), bf16),
            pltpu.VMEM((d, side), bf16),
            pltpu.VMEM((n_tp * side, width), bf16),
            pltpu.VMEM((cap, width), bf16),
            pltpu.VMEM((n_tp, cap, width), bf16),
            pltpu.VMEM((cap, ff), f32),
            pltpu.VMEM((cap, ff), f32),
            pltpu.VMEM((cap, ff), bf16),
            pltpu.VMEM((2, tok_rows, cap), bf16),
            pltpu.VMEM((n_tp, tok_rows, side), bf16),
            pltpu.VMEM((4, cap, width), bf16),
            pltpu.VMEM((cap, width), bf16),
            pltpu.VMEM((cap, width), bf16),
            pltpu.VMEM((cap, width), bf16),
            pltpu.VMEM((cap, width), bf16),
            pltpu.VMEM((cap, width), bf16),
            pltpu.VMEM((cap, width), bf16),
            pltpu.SemaphoreType.DMA((6,)),
            pltpu.SemaphoreType.DMA((n_sends,)),
            pltpu.SemaphoreType.DMA((n_ep,)),
            pltpu.SemaphoreType.DMA((3, n_ep)),
            pltpu.SemaphoreType.DMA((4,)),
            pltpu.SemaphoreType.DMA((n_ep,)),
            pltpu.SemaphoreType.DMA((n_ep,)),
            pltpu.SemaphoreType.DMA((n_ep,)),
            pltpu.SemaphoreType.DMA((n_ep,)),
        ],
        compiler_params=pltpu.CompilerParams(collective_id=0, has_side_effects=True),
    )(
        tokens,
        gate_proj,
        up_proj,
        down_proj,
        side_input_weight,
        dense_out,
        dense_gate,
        chosen_rows,
        choice_weights,
    ).astype(bf16)


def per_device(*args):
    tokens, gate_proj, chosen_rows = args[0], args[1], args[7]
    n_ep, slot = chosen_rows.shape
    n_tp = lax.axis_size("tp")
    width, tile = tokens.shape[1] // n_tp, 2 * LANES
    fits = (
        n_tp == 4
        and n_ep % 4 == 0
        and tokens.shape[0] == n_ep * slot
        and slot % 16 == 0
        and width % tile == 0
        and gate_proj.shape[2] % tile == 0
        and args[4].shape[1] % LANES == 0
    )
    return fused_per_device(*args) if fits else plain_per_device(*args)


def solution(mesh):
    placed = (
        P("ep", None),
        P("ep", None, "tp"),
        P("ep", None, "tp"),
        P("ep", "tp", None),
        P(None, "tp"),
        P(None, "tp"),
        P(),
        P(None, "ep"),
        P(None, "ep"),
    )
    return jax.shard_map(
        per_device, mesh=mesh, in_specs=placed, out_specs=P("ep", "tp"), check_vma=False
    )
```

```python
import functools

import jax
import jax.numpy as jnp
from jax import lax
from jax.experimental import pallas as pl
from jax.experimental.pallas import tpu as pltpu
from jax.sharding import PartitionSpec as P

MESH = pl.DeviceIdType.MESH
LANES = 128


def plain_per_device(
    tokens,
    gate_proj,
    up_proj,
    down_proj,
    side_input_weight,
    dense_out,
    dense_gate,
    chosen_rows,
    choice_weights,
):
    tok_rows = tokens.shape[0]
    width = tokens.shape[1] // lax.axis_size("tp")
    column_position = lax.axis_index("tp") * width
    own_cols = lax.dynamic_slice_in_dim(tokens, column_position, width, 1)
    expert_count, slot_rows = chosen_rows.shape
    capacity = expert_count * slot_rows
    picked = jnp.take(own_cols, chosen_rows.reshape(-1), axis=0).reshape(
        expert_count, slot_rows, width
    )
    arrived = lax.all_to_all(picked, "ep", split_axis=0, concat_axis=1, tiled=True).reshape(
        capacity, width
    )
    piece = lax.all_gather(arrived, "tp", axis=1, tiled=True)
    gate_val = jnp.dot(piece, gate_proj[0], preferred_element_type=jnp.float32)
    up_val = jnp.dot(piece, up_proj[0], preferred_element_type=jnp.float32)
    hidden = (jax.nn.silu(gate_val) * up_val).astype(jnp.bfloat16)
    summed = lax.psum_scatter(
        lax.dot_general(
            down_proj[0], hidden, (((0,), (1,)), ((), ())), preferred_element_type=jnp.float32
        ).astype(jnp.bfloat16),
        "tp",
        scatter_dimension=0,
        tiled=True,
    )
    returned = lax.all_to_all(summed, "ep", split_axis=1, concat_axis=1, tiled=True)
    hits = (
        chosen_rows.reshape(-1)[:, None] == jnp.arange(tok_rows, dtype=jnp.int32)[None, :]
    ).astype(jnp.bfloat16)
    scaled = returned.astype(jnp.float32) * choice_weights.reshape(-1)[None, :]
    high_part = scaled.astype(jnp.bfloat16)
    lower_half = (scaled - high_part.astype(jnp.float32)).astype(jnp.bfloat16)
    contract = (((0,), (1,)), ((), ()))
    routed = lax.dot_general(
        hits, high_part, contract, preferred_element_type=jnp.float32
    ) + lax.dot_general(hits, lower_half, contract, preferred_element_type=jnp.float32)
    dense_hidden = jax.nn.silu(
        jnp.dot(tokens, side_input_weight, preferred_element_type=jnp.float32)
    ).astype(jnp.bfloat16)
    dense_val = jnp.dot(
        lax.all_gather(dense_hidden, "tp", axis=1, tiled=True),
        dense_out,
        preferred_element_type=jnp.float32,
    )
    side_gate = jax.nn.sigmoid(jnp.dot(tokens, dense_gate, preferred_element_type=jnp.float32))
    return (routed + side_gate[:, None] * dense_val).astype(jnp.bfloat16)


def dot(a, b):
    return jnp.dot(a, b, preferred_element_type=jnp.float32)


def silu(v):
    return v / (1.0 + jnp.exp(-v))


def layer_kernel(
    n_ep,
    slot,
    tok_hbm,
    gate_hbm,
    up_hbm,
    down_hbm,
    side_hbm,
    dout_hbm,
    dgate_ref,
    rows_ref,
    cw_ref,
    out_ref,
    tok,
    w_gate,
    w_up,
    w_down,
    w_side,
    w_dout,
    pick,
    xin,
    g_acc,
    u_acc,
    hid,
    comb,
    dhid,
    part,
    d_in,
    rx,
    ry,
    pair,
    fin,
    back,
    load_sem,
    send_sem,
    z_sem,
    ag_sem,
    dh_sem,
    rsd_sem,
    rsx_sem,
    rsy_sem,
    ret_sem,
):
    e = lax.axis_index("ep")
    p = lax.axis_index("tp")
    px = p + 1 - 2 * (p % 2)
    py = p + 2 - 4 * (p // 2)
    pd = px + 2 - 4 * (px // 2)
    z = e // 2
    nz = n_ep // 2
    width = xin.shape[2]
    tok_rows = tok.shape[0]
    side = w_side.shape[1]
    to_x, to_y = {"tp": px}, {"tp": py}

    loads = []
    for i, (src, dst) in enumerate(
        (
            (tok_hbm, tok),
            (side_hbm, w_side),
            (gate_hbm.at[0], w_gate),
            (up_hbm.at[0], w_up),
            (down_hbm.at[0], w_down),
            (dout_hbm, w_dout),
        )
    ):
        copy = pltpu.make_async_copy(src, dst, load_sem.at[i])
        copy.start()
        loads.append(copy)

    barrier = pltpu.get_barrier_semaphore()
    for k in range(1, n_ep):
        pl.semaphore_signal(
            barrier, inc=1, device_id={"ep": (e + k) % n_ep}, device_id_type=MESH
        )
    for there in (to_x, to_y):
        pl.semaphore_signal(barrier, inc=1, device_id=there, device_id_type=MESH)

    def block(owner):
        return pl.ds(pl.multiple_of(owner * slot, slot), slot)

    sends = []

    def send(src, dst, sem, there):
        copy = pltpu.make_async_remote_copy(
            src_ref=src,
            dst_ref=dst,
            send_sem=send_sem.at[len(sends)],
            recv_sem=sem,
            device_id=there,
            device_id_type=MESH,
        )
        copy.start()
        sends.append(copy)

    def arrive(dst, sem):
        pltpu.make_async_remote_copy(
            src_ref=dst,
            dst_ref=dst,
            send_sem=send_sem.at[0],
            recv_sem=sem,
            device_id=to_x,
            device_id_type=MESH,
        ).wait_recv()

    rows_t = rows_ref[...].astype(jnp.float32).T
    cw_t = cw_ref[...].T
    lane = lax.broadcasted_iota(jnp.int32, (slot, tok_rows), 1).astype(jnp.float32)
    hits = jnp.concatenate(
        [jnp.where(rows_t[:, k : k + 1] == lane, 1.0, 0.0) for k in range(n_ep)], axis=0
    )
    loads[0].wait()
    own = pl.ds(pl.multiple_of(p * width, width), width)
    pick[...] = dot(hits.astype(jnp.bfloat16), tok[:, own]).astype(jnp.bfloat16)
    pl.semaphore_wait(barrier, n_ep + 1)

    if nz == 4:
        upper = z // 2
        inner = (z + upper) % 2
        chips = [z, z + 1 - 2 * (z % 2), 2 - upper, 3 - 3 * upper]
        goals = chips
        places = [0, 1, 3 - inner, 3 - inner]
        turn = [2, 3, 1, 0]
    else:
        chips = [(z + nz - g) % nz for g in range(nz)]
        goals = [(z + g) % nz for g in range(nz)]
        places = list(range(nz))
        turn = [*range(1, nz), 0]
    core = e % 2
    partner = e + 1 - 2 * core

    def at(pos):
        return pl.ds(pl.multiple_of(pos * slot, slot), slot)

    send(pick.at[block(partner)], xin.at[p, at(1)], z_sem.at[1], {"ep": partner})
    for g in range(1, nz):
        for c in range(2):
            peer = 2 * goals[g] + c
            mine = 2 * places[g] + core
            send(pick.at[block(peer)], xin.at[p, at(mine)], z_sem.at[mine], {"ep": peer})
    xin[p, at(0)] = pick[block(e), :]

    def spread(pos):
        ref = xin.at[p, at(pos)]
        send(ref, ref, ag_sem.at[0, pos], to_x)
        send(ref, ref, ag_sem.at[1, pos], to_y)

    def forward(pos):
        if pos % 2 == 0:
            ref = xin.at[px, at(pos)]
            arrive(ref, ag_sem.at[0, pos])
            send(ref, ref, ag_sem.at[2, pos], to_y)
        else:
            ref = xin.at[py, at(pos)]
            arrive(ref, ag_sem.at[1, pos])
            send(ref, ref, ag_sem.at[2, pos], to_x)

    spread(0)
    loads[1].wait()
    dhid[p] = silu(dot(tok[...], w_side[...])).astype(jnp.bfloat16)
    arrive(xin.at[p, at(1)], z_sem.at[1])
    spread(1)
    send(dhid.at[p], dhid.at[p], dh_sem.at[0], to_x)
    send(dhid.at[p], dhid.at[p], dh_sem.at[1], to_y)

    weight = jnp.concatenate([cw_t[:, k : k + 1] for k in range(n_ep)], axis=0)
    both = (hits * weight).T
    high = both.astype(jnp.bfloat16)
    comb[0] = high
    comb[1] = (both - high.astype(jnp.float32)).astype(jnp.bfloat16)

    tile = 2 * LANES
    n_tiles = g_acc.shape[1] // tile
    f32 = jnp.float32
    half = tok_rows // 2

    def gate_up(q, first):
        rows = pl.ds(pl.multiple_of(q * width, width), width)

        @pl.loop(0, n_tiles)
        def _(n):
            cols = pl.ds(pl.multiple_of(n * tile, tile), tile)
            g = dot(xin[q], w_gate[rows, cols])
            u = dot(xin[q], w_up[rows, cols])
            if first:
                g_acc[:, cols] = g
                u_acc[:, cols] = u
            else:
                g_acc[:, cols] += g
                u_acc[:, cols] += u

    def gate_up_last(q):
        rows = pl.ds(pl.multiple_of(q * width, width), width)

        @pl.loop(0, n_tiles)
        def _(n):
            cols = pl.ds(pl.multiple_of(n * tile, tile), tile)
            g = g_acc[:, cols] + dot(xin[q], w_gate[rows, cols])
            u = u_acc[:, cols] + dot(xin[q], w_up[rows, cols])
            hid[:, cols] = (silu(g) * u).astype(jnp.bfloat16)

    def down(to, q):

        @pl.loop(0, width // tile)
        def _(n):
            cols = pl.ds(pl.multiple_of(n * tile, tile), tile)
            src = pl.ds(pl.multiple_of(q * width + n * tile, tile), tile)
            part[to, :, cols] = dot(hid[...], w_down[:, src]).astype(jnp.bfloat16)

    def wait_x():
        for pos in range(n_ep):
            if pos % 2:
                arrive(xin.at[px, at(pos)], ag_sem.at[0, pos])

    def wait_y():
        for pos in range(n_ep):
            if pos % 2 == 0:
                arrive(xin.at[py, at(pos)], ag_sem.at[1, pos])

    def wait_d():
        for pos in range(n_ep):
            arrive(xin.at[pd, at(pos)], ag_sem.at[2, pos])

    def first_d(g):
        even, odd = at(2 * g), at(2 * g + 1)
        send(part.at[3, odd], d_in.at[odd], rsd_sem.at[2 * g + 1], to_x)
        send(part.at[3, even], d_in.at[even], rsd_sem.at[2 * g], to_y)

    def direct_x(g):
        odd = at(2 * g + 1)
        send(part.at[1, odd], rx.at[odd], rsx_sem.at[2 * g + 1], to_x)

    def direct_y(g):
        even = at(2 * g)
        send(part.at[2, even], ry.at[even], rsy_sem.at[2 * g], to_y)

    def joined(g):
        for pos, src, dst, sem, there in (
            (2 * g, 1, rx, rsx_sem, to_x),
            (2 * g + 1, 2, ry, rsy_sem, to_y),
        ):
            b = at(pos)
            arrive(d_in.at[b], rsd_sem.at[pos])
            pair[b, :] = (part[src, b, :].astype(f32) + d_in[b, :].astype(f32)).astype(
                jnp.bfloat16
            )
            send(pair.at[b], dst.at[b], sem.at[pos], there)

    def finish(g):
        for c in range(2):
            pos = 2 * g + c
            b = at(pos)
            arrive(rx.at[b], rsx_sem.at[pos])
            arrive(ry.at[b], rsy_sem.at[pos])
            total = (
                part[0, b, :].astype(f32) + rx[b, :].astype(f32) + ry[b, :].astype(f32)
            ).astype(jnp.bfloat16)
            if pos == 0:
                back[block(e), :] = total
            else:
                fin[b, :] = total
                owner = partner if g == 0 else 2 * chips[g] + c
                send(fin.at[b], back.at[block(e)], ret_sem.at[e], {"ep": owner})

    lag = n_ep
    for pos in range(2, n_ep):
        arrive(xin.at[p, at(pos)], z_sem.at[pos])
        spread(pos)
        if pos >= lag:
            forward(pos - lag)
    loads[2].wait()
    loads[3].wait()
    gate_up(p, True)
    for pos in range(n_ep - lag, n_ep):
        forward(pos)
    arrive(dhid.at[px], dh_sem.at[0])
    ref = dhid.at[px, pl.ds(0, half)]
    send(ref, ref, dh_sem.at[2], to_y)
    arrive(dhid.at[py], dh_sem.at[1])
    ref = dhid.at[py, pl.ds(half, half)]
    send(ref, ref, dh_sem.at[3], to_x)
    wait_x()
    gate_up(px, False)
    wait_y()
    gate_up(py, False)
    wait_d()
    gate_up_last(pd)

    loads[4].wait()
    down(3, pd)
    first_d(turn[0])
    first_d(turn[1])
    down(1, px)
    direct_x(turn[0])
    down(2, py)
    direct_y(turn[0])
    direct_x(turn[1])
    direct_y(turn[1])
    down(0, p)
    for i in range(nz):
        joined(turn[i])
        if i + 2 < nz:
            first_d(turn[i + 2])
            direct_x(turn[i + 2])
            direct_y(turn[i + 2])
        if i == 1:
            arrive(dhid.at[pd, pl.ds(0, half)], dh_sem.at[2])
            arrive(dhid.at[pd, pl.ds(half, half)], dh_sem.at[3])
            loads[5].wait()
            total = dot(dhid[0], w_dout[pl.ds(0, side)])
            for q in range(1, dhid.shape[0]):
                total += dot(dhid[q], w_dout[pl.ds(q * side, side)])
            logit = jnp.sum(
                tok[...].astype(f32) * dgate_ref[...].reshape(1, tok.shape[1]).astype(f32),
                axis=1,
                keepdims=True,
            )
            g_acc[:, pl.ds(0, width)] = total / (1.0 + jnp.exp(-logit))
        if i >= 1:
            finish(turn[i - 1])
    finish(turn[-1])

    for k in range(1, n_ep):
        owner = (e + n_ep - k) % n_ep
        arrive(back.at[block(owner)], ret_sem.at[owner])
    out_ref[...] = (
        g_acc[:, pl.ds(0, width)] + dot(comb[0], back[...]) + dot(comb[1], back[...])
    )
    for copy in sends:
        copy.wait_send()


def fused_per_device(
    tokens,
    gate_proj,
    up_proj,
    down_proj,
    side_input_weight,
    dense_out,
    dense_gate,
    chosen_rows,
    choice_weights,
):
    n_ep, slot = chosen_rows.shape
    n_tp = lax.axis_size("tp")
    tok_rows, d = tokens.shape
    width = d // n_tp
    ff = gate_proj.shape[2]
    side = side_input_weight.shape[1]
    cap = n_ep * slot
    bf16, f32 = jnp.bfloat16, jnp.float32
    n_sends = 2 * (n_ep - 1) + 2 * n_ep + n_ep + 4 + 3 * n_ep
    hbm = pl.BlockSpec(memory_space=pltpu.HBM)
    vmem = pl.BlockSpec(memory_space=pltpu.VMEM)
    return pl.pallas_call(
        functools.partial(layer_kernel, n_ep, slot),
        out_shape=pltpu.VMEM((tok_rows, width), f32),
        in_specs=[hbm] * 6 + [vmem] * 3,
        out_specs=vmem,
        scratch_shapes=[
            pltpu.VMEM((tok_rows, d), bf16),
            pltpu.VMEM((d, ff), bf16),
            pltpu.VMEM((d, ff), bf16),
            pltpu.VMEM((ff, d), bf16),
            pltpu.VMEM((d, side), bf16),
            pltpu.VMEM((n_tp * side, width), bf16),
            pltpu.VMEM((cap, width), bf16),
            pltpu.VMEM((n_tp, cap, width), bf16),
            pltpu.VMEM((cap, ff), f32),
            pltpu.VMEM((cap, ff), f32),
            pltpu.VMEM((cap, ff), bf16),
            pltpu.VMEM((2, tok_rows, cap), bf16),
            pltpu.VMEM((n_tp, tok_rows, side), bf16),
            pltpu.VMEM((4, cap, width), bf16),
            pltpu.VMEM((cap, width), bf16),
            pltpu.VMEM((cap, width), bf16),
            pltpu.VMEM((cap, width), bf16),
            pltpu.VMEM((cap, width), bf16),
            pltpu.VMEM((cap, width), bf16),
            pltpu.VMEM((cap, width), bf16),
            pltpu.SemaphoreType.DMA((6,)),
            pltpu.SemaphoreType.DMA((n_sends,)),
            pltpu.SemaphoreType.DMA((n_ep,)),
            pltpu.SemaphoreType.DMA((3, n_ep)),
            pltpu.SemaphoreType.DMA((4,)),
            pltpu.SemaphoreType.DMA((n_ep,)),
            pltpu.SemaphoreType.DMA((n_ep,)),
            pltpu.SemaphoreType.DMA((n_ep,)),
            pltpu.SemaphoreType.DMA((n_ep,)),
        ],
        compiler_params=pltpu.CompilerParams(collective_id=0, has_side_effects=True),
    )(
        tokens,
        gate_proj,
        up_proj,
        down_proj,
        side_input_weight,
        dense_out,
        dense_gate,
        chosen_rows,
        choice_weights,
    ).astype(bf16)


def per_device(*args):
    tokens, gate_proj, chosen_rows = args[0], args[1], args[7]
    n_ep, slot = chosen_rows.shape
    n_tp = lax.axis_size("tp")
    width, tile = tokens.shape[1] // n_tp, 2 * LANES
    fits = (
        n_tp == 4
        and n_ep % 4 == 0
        and tokens.shape[0] == n_ep * slot
        and slot % 16 == 0
        and width % tile == 0
        and gate_proj.shape[2] % tile == 0
        and args[4].shape[1] % LANES == 0
    )
    return fused_per_device(*args) if fits else plain_per_device(*args)


def solution(mesh):
    placed = (
        P("ep", None),
        P("ep", None, "tp"),
        P("ep", None, "tp"),
        P("ep", "tp", None),
        P(None, "tp"),
        P(None, "tp"),
        P(),
        P(None, "ep"),
        P(None, "ep"),
    )
    return jax.shard_map(
        per_device, mesh=mesh, in_specs=placed, out_specs=P("ep", "tp"), check_vma=False
    )
```
